32 devices in a mesh: grp: 2 (over x), kv: 4 (over z), tp: 4 (over y, core).
Axes of the slice: x: 2, y: 2, z: 4, core: 2. Of those that a mesh axis runs over, the one named last changes fastest.
Arguments:
- stream: bfloat16 [32, 4096], P('grp', ('kv', 'tp')), parts along dimension 0, may hold values from -6 to 6
- attn_gain: bfloat16 [4096], P('kv'), may hold values from 0.099609375 to 1.8984375
- mlp_gain: bfloat16 [4096], P('kv'), may hold values from 0.099609375 to 1.8984375
- w_query: bfloat16 [4096, 4096], P('kv', 'tp'), may hold values from -0.09375 to 0.09375
- w_key: bfloat16 [4096, 4096], P('kv', 'tp'), may hold values from -0.09375 to 0.09375
- w_value: bfloat16 [4096, 4096], P('kv', 'tp'), may hold values from -0.09375 to 0.09375
- w_zgate: bfloat16 [4096, 4096], P('kv', 'tp'), may hold values from -0.09375 to 0.09375
- w_decay: bfloat16 [4096, 32], P('kv'), may hold values from -0.09375 to 0.09375
- w_beta: bfloat16 [4096, 32], P('kv'), may hold values from -0.09375 to 0.09375
- decay_rate: float32 [32], P('tp'), may hold values from 0.03 to 3
- head_gain: float32 [128], replicated, may hold values from 0.1 to 1.9
- w_attn_out: bfloat16 [4096, 4096], P('tp', 'kv'), may hold values from -0.09375 to 0.09375
- w_gate: bfloat16 [4096, 11264], P('kv', 'tp'), may hold values from -0.09375 to 0.09375
- w_up: bfloat16 [4096, 11264], P('kv', 'tp'), may hold values from -0.09375 to 0.09375
- w_down: bfloat16 [11264, 4096], P('tp', 'kv'), may hold values from -0.0546875 to 0.0546875
- state: float32 [32, 32, 128, 128], P(('grp', 'kv'), 'tp'), parts along dimension 0, may hold values from -4 to 4
Outputs:
- next_stream: bfloat16 [32, 4096], P('grp', ('kv', 'tp')), parts along dimension 0
- new_state: float32 [32, 32, 128, 128], P(('grp', 'kv'), 'tp'), parts along dimension 0
The draws below stay inside these ranges and needn't reach their ends.
There are 2 independent parts, one for each index of `grp`. The reference program is written for one: setup_inputs(seed, part) draws one part's arguments, and reference() takes and returns one part's arrays. A program takes and returns all parts, laid end to end along the dimension named above; an argument that names none is the same for every part. Nothing has to cross between parts.
All inputs are finite; a program needn't handle non-finite values.
Results may differ from the reference program's by a relative error of at most 0.025.
Values may be sent and summed in bfloat16 or wider, within the bound.
A program may use at most 64 MiB of HBM per device.

```python
import math
import jax
import jax.numpy as jnp
from jax import lax

D = 4096
HEADS = 32
HEAD_DIM = 128
FF = 11264
BATCH = 16


def block_scale(rng, dims, pieces, least, top_value):
    level = 1.0
    for axis_at, parts in pieces:
        steps = jax.random.uniform(jax.random.fold_in(jax.random.fold_in(rng, 6), axis_at), (parts,), jnp.float32, least / len(pieces), top_value / len(pieces))
        level = level * jnp.repeat(jnp.exp(steps), dims[axis_at] // parts).reshape((-1,) + (1,) * (len(dims) - 1 - axis_at))
    return level


def centred(rng, extent, width, bound, split=(), dtype=jnp.bfloat16):
    result = width * jax.random.normal(rng, extent, jnp.float32)
    if split:
        result = result * block_scale(rng, extent, split, -0.22, 0.18)
    return jnp.clip(result, -bound, bound).astype(dtype)


def setup_inputs(seed: int = 0, part: int = 0) -> dict:
    seeds = jax.random.split(jax.random.key(seed), 17)
    own_keys = jax.random.split(jax.random.fold_in(seeds[16], part), 17)
    return {
        "stream": centred(own_keys[0], (BATCH, D), 1.0, 6.0, ((1, 16),)),
        "attn_gain": jnp.clip(1.0 + 0.18 * jax.random.normal(seeds[1], (D,), jnp.float32), 0.099609375, 1.8984375).astype(jnp.bfloat16),
        "mlp_gain": jnp.clip(1.0 + 0.18 * jax.random.normal(seeds[2], (D,), jnp.float32), 0.099609375, 1.8984375).astype(jnp.bfloat16),
        "w_query": centred(seeds[3], (D, HEADS * HEAD_DIM), D ** -0.5, 0.09375, ((0, 4), (1, 4))),
        "w_key": centred(seeds[4], (D, HEADS * HEAD_DIM), D ** -0.5, 0.09375, ((0, 4), (1, 4))),
        "w_value": centred(seeds[5], (D, HEADS * HEAD_DIM), D ** -0.5, 0.09375, ((0, 4), (1, 4))),
        "w_zgate": centred(seeds[6], (D, HEADS * HEAD_DIM), D ** -0.5, 0.09375, ((0, 4), (1, 4))),
        "w_decay": centred(seeds[7], (D, HEADS), D ** -0.5, 0.09375, ((0, 4),)),
        "w_beta": centred(seeds[8], (D, HEADS), D ** -0.5, 0.09375, ((0, 4),)),
        "decay_rate": jnp.clip(jnp.exp(math.log(3.0) - 4.6051702 * jax.random.uniform(seeds[9], (HEADS,), jnp.float32) ** block_scale(seeds[9], (HEADS,), ((0, 4),), -0.2, 0.2)), 0.03, 3.0),
        "head_gain": jnp.clip(1.0 + 0.18 * jax.random.normal(seeds[10], (HEAD_DIM,), jnp.float32), 0.1, 1.9),
        "w_attn_out": centred(seeds[11], (HEADS * HEAD_DIM, D), (HEADS * HEAD_DIM) ** -0.5, 0.09375, ((0, 4), (1, 4))),
        "w_gate": centred(seeds[12], (D, FF), D ** -0.5, 0.09375, ((0, 4), (1, 4))),
        "w_up": centred(seeds[13], (D, FF), D ** -0.5, 0.09375, ((0, 4), (1, 4))),
        "w_down": centred(seeds[14], (FF, D), FF ** -0.5, 0.0546875, ((0, 4), (1, 4))),
        "state": centred(own_keys[15], (BATCH, HEADS, HEAD_DIM, HEAD_DIM), 0.3, 4.0, ((0, 4), (1, 4)), jnp.float32),
    }


EPSILON = 1e-06

def l2_unit(values):
    return values * lax.rsqrt(lax.optimization_barrier(jnp.sum(values * values, axis=-1, keepdims=True)) + EPSILON)

def delta_update(query, key_vec, value_vec, log_decay, beta_gate, state):
    decayed = jnp.exp(log_decay)[..., None, None] * state
    recalled = jnp.einsum('shkv,shk->shv', decayed, key_vec, precision=lax.Precision.HIGHEST)
    update = beta_gate[..., None] * (value_vec - recalled)
    new_state = decayed + key_vec[..., :, None] * update[..., None, :]
    head_out = jnp.einsum('shkv,shk->shv', new_state, query, precision=lax.Precision.HIGHEST)
    return (new_state, head_out)

def head_mix(head_out, head_gain, z_gate):
    scaled = head_out * lax.rsqrt(lax.optimization_barrier(jnp.mean(head_out * head_out, axis=-1, keepdims=True)) + EPSILON)
    return (scaled * head_gain.astype(jnp.float32) * jax.nn.silu(z_gate)).astype(jnp.bfloat16)

def reference(stream, attn_gain, mlp_gain, w_query, w_key, w_value, w_zgate, w_decay, w_beta, decay_rate, head_gain, w_attn_out, w_gate, w_up, w_down, state):
    batch = stream.shape[0]
    stream_f = stream.astype(jnp.float32)
    row_scale = lax.rsqrt(lax.optimization_barrier(jnp.mean(stream_f * stream_f, axis=1, keepdims=True)) + EPSILON)
    normed = (stream_f * attn_gain.astype(jnp.float32)[None, :]).astype(jnp.bfloat16)

    def project(weight):
        return jnp.dot(normed, weight, preferred_element_type=jnp.float32) * row_scale
    query = l2_unit(project(w_query).reshape(batch, HEADS, HEAD_DIM)) * HEAD_DIM ** (-0.5)
    key_vec = l2_unit(project(w_key).reshape(batch, HEADS, HEAD_DIM))
    value_vec = project(w_value).reshape(batch, HEADS, HEAD_DIM)
    z_gate = project(w_zgate).reshape(batch, HEADS, HEAD_DIM)
    log_decay = -decay_rate[None, :] * jax.nn.softplus(project(w_decay))
    beta_gate = jax.nn.sigmoid(project(w_beta))
    new_state, head_out = delta_update(query, key_vec, value_vec, log_decay, beta_gate, state)
    mixed = head_mix(head_out, head_gain, z_gate).reshape(batch, HEADS * HEAD_DIM)
    residual_stream = (stream_f + jnp.dot(mixed, w_attn_out, preferred_element_type=jnp.float32)).astype(jnp.bfloat16)
    resid_f = residual_stream.astype(jnp.float32)
    mlp_scale = lax.rsqrt(lax.optimization_barrier(jnp.mean(resid_f * resid_f, axis=1, keepdims=True)) + EPSILON)
    normed_mlp = (resid_f * mlp_gain.astype(jnp.float32)[None, :]).astype(jnp.bfloat16)
    gate = jnp.dot(normed_mlp, w_gate, preferred_element_type=jnp.float32) * mlp_scale
    up_proj = jnp.dot(normed_mlp, w_up, preferred_element_type=jnp.float32) * mlp_scale
    hidden = (jax.nn.silu(gate) * up_proj).astype(jnp.bfloat16)
    next_stream = (resid_f + jnp.dot(hidden, w_down, preferred_element_type=jnp.float32)).astype(jnp.bfloat16)
    return (next_stream, new_state)
```

```python
import functools
import math

import jax
import jax.numpy as jnp
from jax import lax
from jax.experimental import pallas as pl
from jax.experimental.pallas import tpu as pltpu
from jax.sharding import PartitionSpec as P

D = 4096
HEAD_DIM = 128


EPSILON = 1e-06


def l2_unit(values):
    return values * lax.rsqrt(jnp.sum(values * values, axis=-1, keepdims=True) + EPSILON)


def delta_update(query, key_vec, value_vec, log_decay, beta_gate, state):
    decayed = jnp.exp(log_decay)[..., None, None] * state
    recalled = jnp.einsum("shkv,shk->shv", decayed, key_vec, precision=lax.Precision.HIGHEST)
    update = beta_gate[..., None] * (value_vec - recalled)
    new_state = decayed + key_vec[..., :, None] * update[..., None, :]
    head_out = jnp.einsum("shkv,shk->shv", new_state, query, precision=lax.Precision.HIGHEST)
    return (new_state, head_out)


def head_mix(head_out, head_gain, z_gate):
    scaled = head_out * lax.rsqrt(jnp.mean(head_out * head_out, axis=-1, keepdims=True) + EPSILON)
    return (scaled * head_gain * jax.nn.silu(z_gate)).astype(jnp.bfloat16)


def local(
    stream,
    attn_gain,
    mlp_gain,
    w_query,
    w_key,
    w_value,
    w_zgate,
    w_decay,
    w_beta,
    decay_rate,
    head_gain,
    w_attn_out,
    w_gate,
    w_up,
    w_down,
    state,
):
    seq_count = state.shape[0]
    local_heads = state.shape[1]
    width = w_query.shape[1]
    heads_total = w_decay.shape[1]
    kv_offset = lax.axis_index("kv") * seq_count
    head_offset = lax.axis_index("tp") * local_heads
    block_rows = lax.all_gather(stream, "tp", axis=1, tiled=True).astype(jnp.float32)
    local_squares = jnp.sum(block_rows * block_rows, axis=1)
    normed = (block_rows * attn_gain.astype(jnp.float32)[None, :]).astype(jnp.bfloat16)
    small_weights = jnp.concatenate([w_decay, w_beta], axis=1)
    pieces = [
        jnp.dot(normed, weight, preferred_element_type=jnp.float32)
        for weight in (w_query, w_key, w_value, w_zgate)
    ]
    small = jnp.dot(normed, small_weights, preferred_element_type=jnp.float32)
    own_decay = lax.dynamic_slice_in_dim(small, head_offset, local_heads, 1)
    own_beta = lax.dynamic_slice_in_dim(small, heads_total + head_offset, local_heads, 1)
    summed = lax.psum_scatter(
        jnp.concatenate(pieces + [own_decay, own_beta], axis=1).astype(jnp.bfloat16),
        "kv",
        scatter_dimension=0,
        tiled=True,
    ).astype(jnp.float32)
    total_squares = lax.psum(local_squares, "kv")
    row_scale = lax.rsqrt(total_squares / D + EPSILON)
    own_scale = lax.dynamic_slice_in_dim(row_scale, kv_offset, seq_count, 0)
    summed = summed * own_scale[:, None]

    def head_block(index):
        return summed[:, index * width : (index + 1) * width].reshape(
            seq_count, local_heads, HEAD_DIM
        )

    query = l2_unit(head_block(0)) * HEAD_DIM ** (-0.5)
    key_vec = l2_unit(head_block(1))
    value_vec = head_block(2)
    z_gate = head_block(3)
    log_decay = -decay_rate[None, :] * jax.nn.softplus(
        summed[:, 4 * width : 4 * width + local_heads]
    )
    beta_gate = jax.nn.sigmoid(summed[:, 4 * width + local_heads :])
    new_state, head_out = delta_update(query, key_vec, value_vec, log_decay, beta_gate, state)
    mixed = head_mix(head_out, head_gain, z_gate).reshape(seq_count, width)
    attn_part = jnp.dot(
        lax.all_gather(mixed, "kv", axis=0, tiled=True),
        w_attn_out,
        preferred_element_type=jnp.float32,
    )
    attn_sum = lax.psum_scatter(
        attn_part.astype(jnp.bfloat16), "tp", scatter_dimension=1, tiled=True
    ).astype(jnp.float32)
    residual_stream = (stream.astype(jnp.float32) + attn_sum).astype(jnp.bfloat16)
    mlp_block = lax.all_gather(residual_stream, "tp", axis=1, tiled=True).astype(jnp.float32)
    mlp_local_squares = jnp.sum(mlp_block * mlp_block, axis=1)
    mlp_total_squares = lax.psum(mlp_local_squares, "kv")
    normed_mlp = (mlp_block * mlp_gain.astype(jnp.float32)[None, :]).astype(jnp.bfloat16)
    gate_part = jnp.dot(normed_mlp, w_gate, preferred_element_type=jnp.float32)
    up_part = jnp.dot(normed_mlp, w_up, preferred_element_type=jnp.float32)
    operands = (gate_part, up_part)
    totals = (
        lax.psum(operands[0].astype(jnp.bfloat16), "kv").astype(jnp.float32),
        lax.psum(operands[1].astype(jnp.bfloat16), "kv").astype(jnp.float32),
    )
    gate_sum, up_sum = (totals[0], totals[1])
    mlp_scale = lax.rsqrt(mlp_total_squares / D + EPSILON)
    hidden = (jax.nn.silu(gate_sum * mlp_scale[:, None]) * (up_sum * mlp_scale[:, None])).astype(
        jnp.bfloat16
    )
    down_part = jnp.dot(hidden, w_down, preferred_element_type=jnp.float32)
    mlp_sum = lax.psum_scatter(
        down_part.astype(jnp.bfloat16), "tp", scatter_dimension=1, tiled=True
    ).astype(jnp.float32)
    next_stream = (residual_stream.astype(jnp.float32) + mlp_sum).astype(jnp.bfloat16)
    return (next_stream, new_state)


LANES = 128
VMEM_BYTES = 67043328
MESH = pl.DeviceIdType.MESH


def send_slots(count, axis, me, source, slots, send_sem, recv_sem):
    copies = []
    for step in range(1, count):
        peer = lax.rem(me + step, count)
        copy = pltpu.make_async_remote_copy(
            src_ref=source(peer),
            dst_ref=slots.at[me],
            send_sem=send_sem.at[step],
            recv_sem=recv_sem.at[step],
            device_id={axis: peer},
            device_id_type=MESH,
        )
        copy.start()
        copies.append(copy)
    return copies


def wait_slot(count, axis, me, step, slots, send_sem, recv_sem):
    origin = lax.rem(me + count - step, count)
    pltpu.make_async_remote_copy(
        src_ref=slots.at[origin],
        dst_ref=slots.at[origin],
        send_sem=send_sem.at[step],
        recv_sem=recv_sem.at[step],
        device_id={axis: origin},
        device_id_type=MESH,
    ).wait_recv()
    return origin


def layer_kernel(
    kv_count,
    tp_count,
    stream,
    attn_gain,
    mlp_gain,
    w_query,
    w_key,
    w_value,
    w_zgate,
    w_decay,
    w_beta,
    decay_rate,
    head_gain,
    w_attn_out,
    w_gate,
    w_up,
    w_down,
    state,
    out_stream,
    out_state,
    v_query,
    v_key,
    v_value,
    v_zgate,
    v_decay,
    v_beta,
    v_attn_out,
    v_gate,
    v_up,
    v_down,
    v_state,
    x_all,
    normed,
    proj_f,
    proj_b,
    proj_r,
    proj_t,
    rows,
    mix_all,
    mixed_f,
    part_f,
    part_b,
    part_r,
    res_all,
    gu_f,
    gu_b,
    gu_r,
    gu_t,
    hid_all,
    hidden_f,
    down_f,
    down_b,
    down_r,
    load_sem,
    send_sem,
    recv_sem,
):
    f32, bf16 = jnp.float32, jnp.bfloat16
    kv, tp = lax.axis_index("kv"), lax.axis_index("tp")
    batch, width = stream.shape
    depth, cols = w_query.shape
    seqs, heads = state.shape[0], state.shape[1]
    heads_total = w_decay.shape[1]
    half = w_gate.shape[1] // 2
    features = kv_count * depth

    def load(index, source, target):
        copy = pltpu.make_async_copy(source, target, load_sem.at[index])
        copy.start()
        return copy

    load_x = load(0, stream, x_all.at[tp])
    loads = [
        load(index + 1, source, target)
        for index, (source, target) in enumerate(
            (
                (w_decay, v_decay),
                (w_beta, v_beta),
                (w_query, v_query),
                (w_key, v_key),
                (w_value, v_value),
                (w_zgate, v_zgate),
                (state, v_state),
                (w_attn_out, v_attn_out),
                (w_gate, v_gate),
                (w_up, v_up),
                (w_down, v_down),
            )
        )
    ]
    (l_decay, l_beta, l_query, l_key, l_value, l_zgate) = loads[:6]
    (l_state, l_attn_out, l_gate, l_up, l_down) = loads[6:]

    barrier = pltpu.get_barrier_semaphore()
    for step in range(1, tp_count):
        pl.semaphore_signal(
            barrier, inc=1, device_id={"tp": lax.rem(tp + step, tp_count)}, device_id_type=MESH
        )
    for step in range(1, kv_count):
        pl.semaphore_signal(
            barrier, inc=1, device_id={"kv": lax.rem(kv + step, kv_count)}, device_id_type=MESH
        )
    load_x.wait()
    pl.semaphore_wait(barrier, tp_count - 1 + kv_count - 1)

    def tp_exchange(index, source, slots):
        sends = send_slots(
            tp_count, "tp", tp, source, slots, send_sem.at[index], recv_sem.at[index]
        )

        def arrived(step):
            return wait_slot(
                tp_count, "tp", tp, step, slots, send_sem.at[index], recv_sem.at[index]
            )

        return sends, arrived

    def kv_exchange(index, source, slots):
        sends = send_slots(
            kv_count, "kv", kv, source, slots, send_sem.at[index], recv_sem.at[index]
        )

        def arrived(step):
            return wait_slot(
                kv_count, "kv", kv, step, slots, send_sem.at[index], recv_sem.at[index]
            )

        return sends, arrived

    pending = []

    def norm_inputs(blocks, gain):
        squares = jnp.zeros((batch, 1), f32)
        for t in range(tp_count):
            block = blocks[t].astype(f32)
            squares = squares + jnp.sum(block * block, axis=1, keepdims=True)
            normed[:, t * width : (t + 1) * width] = (
                block * gain[:, t * width : (t + 1) * width].astype(f32)
            ).astype(bf16)
        squares = jnp.broadcast_to(squares, (batch, LANES))
        high = squares.astype(bf16).astype(f32)
        return high, squares - high

    sends, arrived = tp_exchange(0, lambda peer: x_all.at[tp], x_all)
    pending += sends
    for step in range(1, tp_count):
        arrived(step)
    high, low = norm_inputs(x_all, attn_gain)

    inputs = normed[...]
    l_decay.wait()
    l_beta.wait()
    decay_part = jnp.dot(inputs, v_decay[...], preferred_element_type=f32)
    beta_part = jnp.dot(inputs, v_beta[...], preferred_element_type=f32)
    for j in range(kv_count):
        own = slice(j * seqs, (j + 1) * seqs)
        proj_f[j, :, cols:] = jnp.zeros((4 * seqs, LANES), f32)
        proj_f[j, 0:seqs, cols : cols + heads_total] = decay_part[own]
        proj_f[j, seqs : 2 * seqs, cols : cols + heads_total] = beta_part[own]
        proj_f[j, 2 * seqs : 3 * seqs, cols:] = high[own]
        proj_f[j, 3 * seqs : 4 * seqs, cols:] = low[own]
    for kind, (wait, weight) in enumerate(
        ((l_query, v_query), (l_key, v_key), (l_value, v_value), (l_zgate, v_zgate))
    ):
        wait.wait()
        part = jnp.dot(inputs, weight[...], preferred_element_type=f32)
        for j in range(kv_count):
            proj_f[j, kind * seqs : (kind + 1) * seqs, 0:cols] = part[j * seqs : (j + 1) * seqs]
    for j in range(kv_count):
        proj_b[j] = proj_f[j].astype(bf16)
    sends, arrived = kv_exchange(1, lambda peer: proj_b.at[peer], proj_r)
    pending += sends
    total = proj_f[kv]
    for step in range(1, kv_count):
        total = total + proj_r[arrived(step)].astype(f32)
    proj_t[...] = total

    squares = proj_t[2 * seqs : 3 * seqs, cols:] + proj_t[3 * seqs : 4 * seqs, cols:]
    row_scale = lax.rsqrt(squares / features + EPSILON)
    decay_rows = proj_t[0:seqs, cols:] * row_scale
    beta_rows = proj_t[seqs : 2 * seqs, cols:] * row_scale
    for h in range(heads):
        at = slice(h * seqs, (h + 1) * seqs)
        for kind in range(4):
            rows[kind, at, :] = (
                proj_t[kind * seqs : (kind + 1) * seqs, h * LANES : (h + 1) * LANES] * row_scale
            )
        rows[4, at, :] = decay_rows
        rows[5, at, :] = beta_rows
    count = heads * seqs
    row = lax.broadcasted_iota(jnp.int32, (count, LANES), 0)
    lane = lax.broadcasted_iota(jnp.int32, (count, LANES), 1) - tp * heads
    own_lane = (row >= lane * seqs) & (row < (lane + 1) * seqs)
    decay_pre = jnp.sum(jnp.where(own_lane, rows[4], 0.0), axis=1, keepdims=True)
    beta_pre = jnp.sum(jnp.where(own_lane, rows[5], 0.0), axis=1, keepdims=True)
    row = lax.broadcasted_iota(jnp.int32, (count, heads), 0)
    lane = lax.broadcasted_iota(jnp.int32, (count, heads), 1)
    own_lane = (row >= lane * seqs) & (row < (lane + 1) * seqs)
    rate = jnp.sum(
        jnp.where(own_lane, jnp.broadcast_to(decay_rate[...], (count, heads)), 0.0),
        axis=1,
        keepdims=True,
    )
    softplus = jnp.maximum(decay_pre, 0.0) + jnp.log1p(jnp.exp(-jnp.abs(decay_pre)))
    rows[4] = jnp.broadcast_to(jnp.exp(-rate * softplus), (count, LANES))
    rows[5] = jnp.broadcast_to(jax.nn.sigmoid(beta_pre), (count, LANES))
    query_t = jnp.transpose(l2_unit(rows[0]) * HEAD_DIM ** (-0.5))
    key_t = jnp.transpose(l2_unit(rows[1]))

    l_state.wait()
    for h in range(heads):
        for s in range(seqs):
            i = h * seqs + s
            key_col = key_t[:, i : i + 1]
            decayed = v_state[s, h] * rows[4, i : i + 1, :]
            recalled = jnp.sum(decayed * key_col, axis=0, keepdims=True)
            update = rows[5, i : i + 1, :] * (rows[2, i : i + 1, :] - recalled)
            updated = decayed + key_col * update
            v_state[s, h] = updated
            rows[0, i : i + 1, :] = jnp.sum(
                updated * query_t[:, i : i + 1], axis=0, keepdims=True
            )
    head_out = rows[0]
    scaled = head_out * lax.rsqrt(
        jnp.mean(head_out * head_out, axis=-1, keepdims=True) + EPSILON
    )
    mix_all[kv] = (scaled * head_gain[...] * jax.nn.silu(rows[3])).astype(bf16)
    sends, arrived = kv_exchange(2, lambda peer: mix_all.at[kv], mix_all)
    pending += sends
    store_state = pltpu.make_async_copy(v_state, out_state, load_sem.at[len(loads) + 1])
    store_state.start()
    for step in range(1, kv_count):
        arrived(step)
    for j in range(kv_count):
        mixed = mix_all[j].astype(f32)
        for h in range(heads):
            mixed_f[j * seqs : (j + 1) * seqs, h * LANES : (h + 1) * LANES] = mixed[
                h * seqs : (h + 1) * seqs
            ]

    def sum_over_tp(index, part, held, sent, slots):
        for t in range(tp_count):
            block = part[:, t * width : (t + 1) * width]
            held[t] = block
            sent[t] = block.astype(bf16)
        sends, arrived = tp_exchange(index, lambda peer: sent.at[peer], slots)
        total = held[tp]
        for step in range(1, tp_count):
            total = total + slots[arrived(step)].astype(f32)
        return sends, total

    l_attn_out.wait()
    part = jnp.dot(mixed_f[...].astype(bf16), v_attn_out[...], preferred_element_type=f32)
    sends, attn_sum = sum_over_tp(3, part, part_f, part_b, part_r)
    pending += sends
    res_all[tp] = (x_all[tp].astype(f32) + attn_sum).astype(bf16)
    sends, arrived = tp_exchange(4, lambda peer: res_all.at[tp], res_all)
    pending += sends
    for step in range(1, tp_count):
        arrived(step)
    high, low = norm_inputs(res_all, mlp_gain)

    inputs = normed[...]
    for j in range(kv_count):
        own = slice(j * seqs, (j + 1) * seqs)
        gu_f[j, :, half:] = jnp.zeros((4 * seqs, LANES), f32)
        gu_f[j, 0:seqs, half:] = high[own]
        gu_f[j, seqs : 2 * seqs, half:] = low[own]
    for kind, (wait, weight) in enumerate(((l_gate, v_gate), (l_up, v_up))):
        wait.wait()
        for side in range(2):
            part = jnp.dot(
                inputs,
                weight[:, side * half : (side + 1) * half],
                preferred_element_type=f32,
            )
            at = (2 * kind + side) * seqs
            for j in range(kv_count):
                gu_f[j, at : at + seqs, 0:half] = part[j * seqs : (j + 1) * seqs]
    for j in range(kv_count):
        gu_b[j] = gu_f[j].astype(bf16)
    sends, arrived = kv_exchange(5, lambda peer: gu_b.at[peer], gu_r)
    pending += sends
    total = gu_f[kv]
    for step in range(1, kv_count):
        total = total + gu_r[arrived(step)].astype(f32)
    gu_t[...] = total
    squares = gu_t[0:seqs, half:] + gu_t[seqs : 2 * seqs, half:]
    mlp_scale = lax.rsqrt(squares / features + EPSILON)[:, 0:1]
    mlp_scale = jnp.concatenate([mlp_scale, mlp_scale], axis=0)
    gate = gu_t[0 : 2 * seqs, 0:half] * mlp_scale
    up = gu_t[2 * seqs : 4 * seqs, 0:half] * mlp_scale
    hid_all[kv] = (jax.nn.silu(gate) * up).astype(bf16)
    sends, arrived = kv_exchange(6, lambda peer: hid_all.at[kv], hid_all)
    pending += sends
    for step in range(1, kv_count):
        arrived(step)
    for j in range(kv_count):
        hidden = hid_all[j].astype(f32)
        for side in range(2):
            hidden_f[j * seqs : (j + 1) * seqs, side * half : (side + 1) * half] = hidden[
                side * seqs : (side + 1) * seqs
            ]
    l_down.wait()
    part = jnp.dot(hidden_f[...].astype(bf16), v_down[...], preferred_element_type=f32)
    sends, mlp_sum = sum_over_tp(7, part, down_f, down_b, down_r)
    pending += sends
    out_stream[...] = (res_all[tp].astype(f32) + mlp_sum).astype(bf16)
    for copy in pending:
        copy.wait_send()
    store_state.wait()


def fused(kv_count, tp_count, *args):
    f32, bf16 = jnp.float32, jnp.bfloat16
    (stream, attn_gain, mlp_gain, w_query, w_key, w_value, w_zgate, w_decay, w_beta) = args[:9]
    (decay_rate, head_gain, w_attn_out, w_gate, w_up, w_down, state) = args[9:]
    batch, width = stream.shape
    depth, cols = w_query.shape
    seqs, heads = state.shape[0], state.shape[1]
    half = w_gate.shape[1] // 2
    count = seqs * heads
    steps = max(kv_count, tp_count)
    any_spec = pl.BlockSpec(memory_space=pl.ANY)
    vmem_spec = pl.BlockSpec(memory_space=pltpu.VMEM)
    weights = (w_query, w_key, w_value, w_zgate, w_decay, w_beta, w_attn_out, w_gate, w_up, w_down)
    scratch = [pltpu.VMEM(weight.shape, weight.dtype) for weight in weights + (state,)]
    scratch += [
        pltpu.VMEM((tp_count, batch, width), bf16),
        pltpu.VMEM((batch, depth), bf16),
        pltpu.VMEM((kv_count, 4 * seqs, cols + LANES), f32),
        pltpu.VMEM((kv_count, 4 * seqs, cols + LANES), bf16),
        pltpu.VMEM((kv_count, 4 * seqs, cols + LANES), bf16),
        pltpu.VMEM((4 * seqs, cols + LANES), f32),
        pltpu.VMEM((6, count, LANES), f32),
        pltpu.VMEM((kv_count, count, LANES), bf16),
        pltpu.VMEM((batch, cols), f32),
        pltpu.VMEM((tp_count, batch, width), f32),
        pltpu.VMEM((tp_count, batch, width), bf16),
        pltpu.VMEM((tp_count, batch, width), bf16),
        pltpu.VMEM((tp_count, batch, width), bf16),
        pltpu.VMEM((kv_count, 4 * seqs, half + LANES), f32),
        pltpu.VMEM((kv_count, 4 * seqs, half + LANES), bf16),
        pltpu.VMEM((kv_count, 4 * seqs, half + LANES), bf16),
        pltpu.VMEM((4 * seqs, half + LANES), f32),
        pltpu.VMEM((kv_count, 2 * seqs, half), bf16),
        pltpu.VMEM((batch, 2 * half), f32),
        pltpu.VMEM((tp_count, batch, width), f32),
        pltpu.VMEM((tp_count, batch, width), bf16),
        pltpu.VMEM((tp_count, batch, width), bf16),
        pltpu.SemaphoreType.DMA((13,)),
        pltpu.SemaphoreType.DMA((8, steps)),
        pltpu.SemaphoreType.DMA((8, steps)),
    ]
    return pl.pallas_call(
        functools.partial(layer_kernel, kv_count, tp_count),
        out_shape=(
            jax.ShapeDtypeStruct(stream.shape, bf16),
            jax.ShapeDtypeStruct(state.shape, f32),
        ),
        in_specs=[any_spec]
        + [vmem_spec] * 2
        + [any_spec] * 6
        + [vmem_spec] * 2
        + [any_spec] * 5,
        out_specs=(vmem_spec, any_spec),
        scratch_shapes=scratch,
        compiler_params=pltpu.CompilerParams(
            collective_id=0, has_side_effects=True, vmem_limit_bytes=VMEM_BYTES
        ),
    )(
        stream,
        attn_gain.reshape(1, -1),
        mlp_gain.reshape(1, -1),
        w_query,
        w_key,
        w_value,
        w_zgate,
        w_decay,
        w_beta,
        decay_rate.reshape(1, -1),
        head_gain.reshape(1, -1),
        w_attn_out,
        w_gate,
        w_up,
        w_down,
        state,
    )


def layer(mesh, *args):
    kv_count, tp_count = mesh.shape["kv"], mesh.shape["tp"]
    stream, w_query, w_gate, state = args[0], args[3], args[12], args[15]
    seqs, heads = state.shape[0], state.shape[1]
    held = sum(math.prod(a.shape) * a.dtype.itemsize for a in args)
    tiled = (
        stream.shape[1] % LANES == 0
        and w_query.shape[0] == tp_count * stream.shape[1]
        and stream.shape[0] == kv_count * seqs
        and stream.shape[0] % 16 == 0
        and (2 * seqs) % 8 == 0
        and (seqs * heads) % 16 == 0
        and w_gate.shape[1] % (2 * LANES) == 0
        and args[7].shape[1] <= LANES
        and state.shape[2] == LANES
        and state.shape[3] == LANES
        and kv_count > 1
        and tp_count > 1
        and held < VMEM_BYTES * 3 // 4
    )
    if tiled:
        return fused(kv_count, tp_count, *args)
    return local(*args)


def solution(mesh):
    return jax.shard_map(
        functools.partial(layer, mesh),
        mesh=mesh,
        in_specs=(
            P("grp", ("kv", "tp")),
            P("kv"),
            P("kv"),
            P("kv", "tp"),
            P("kv", "tp"),
            P("kv", "tp"),
            P("kv", "tp"),
            P("kv", None),
            P("kv", None),
            P("tp"),
            P(),
            P("tp", "kv"),
            P("kv", "tp"),
            P("kv", "tp"),
            P("tp", "kv"),
            P(("grp", "kv"), "tp", None, None),
        ),
        out_specs=(P("grp", ("kv", "tp")), P(("grp", "kv"), "tp", None, None)),
        check_vma=False,
    )
```

```python
import functools
import math

import jax
import jax.numpy as jnp
from jax import lax
from jax.experimental import pallas as pl
from jax.experimental.pallas import tpu as pltpu
from jax.sharding import PartitionSpec as P

D = 4096
HEAD_DIM = 128


EPSILON = 1e-06


def l2_unit(values):
    return values * lax.rsqrt(jnp.sum(values * values, axis=-1, keepdims=True) + EPSILON)


def delta_update(query, key_vec, value_vec, log_decay, beta_gate, state):
    decayed = jnp.exp(log_decay)[..., None, None] * state
    recalled = jnp.einsum("shkv,shk->shv", decayed, key_vec, precision=lax.Precision.HIGHEST)
    update = beta_gate[..., None] * (value_vec - recalled)
    new_state = decayed + key_vec[..., :, None] * update[..., None, :]
    head_out = jnp.einsum("shkv,shk->shv", new_state, query, precision=lax.Precision.HIGHEST)
    return (new_state, head_out)


def head_mix(head_out, head_gain, z_gate):
    scaled = head_out * lax.rsqrt(jnp.mean(head_out * head_out, axis=-1, keepdims=True) + EPSILON)
    return (scaled * head_gain * jax.nn.silu(z_gate)).astype(jnp.bfloat16)


def local(
    stream,
    attn_gain,
    mlp_gain,
    w_query,
    w_key,
    w_value,
    w_zgate,
    w_decay,
    w_beta,
    decay_rate,
    head_gain,
    w_attn_out,
    w_gate,
    w_up,
    w_down,
    state,
):
    seq_count = state.shape[0]
    local_heads = state.shape[1]
    width = w_query.shape[1]
    heads_total = w_decay.shape[1]
    kv_offset = lax.axis_index("kv") * seq_count
    head_offset = lax.axis_index("tp") * local_heads
    block_rows = lax.all_gather(stream, "tp", axis=1, tiled=True).astype(jnp.float32)
    local_squares = jnp.sum(block_rows * block_rows, axis=1)
    normed = (block_rows * attn_gain.astype(jnp.float32)[None, :]).astype(jnp.bfloat16)
    small_weights = jnp.concatenate([w_decay, w_beta], axis=1)
    pieces = [
        jnp.dot(normed, weight, preferred_element_type=jnp.float32)
        for weight in (w_query, w_key, w_value, w_zgate)
    ]
    small = jnp.dot(normed, small_weights, preferred_element_type=jnp.float32)
    own_decay = lax.dynamic_slice_in_dim(small, head_offset, local_heads, 1)
    own_beta = lax.dynamic_slice_in_dim(small, heads_total + head_offset, local_heads, 1)
    summed = lax.psum_scatter(
        jnp.concatenate(pieces + [own_decay, own_beta], axis=1).astype(jnp.bfloat16),
        "kv",
        scatter_dimension=0,
        tiled=True,
    ).astype(jnp.float32)
    total_squares = lax.psum(local_squares, "kv")
    row_scale = lax.rsqrt(total_squares / D + EPSILON)
    own_scale = lax.dynamic_slice_in_dim(row_scale, kv_offset, seq_count, 0)
    summed = summed * own_scale[:, None]

    def head_block(index):
        return summed[:, index * width : (index + 1) * width].reshape(
            seq_count, local_heads, HEAD_DIM
        )

    query = l2_unit(head_block(0)) * HEAD_DIM ** (-0.5)
    key_vec = l2_unit(head_block(1))
    value_vec = head_block(2)
    z_gate = head_block(3)
    log_decay = -decay_rate[None, :] * jax.nn.softplus(
        summed[:, 4 * width : 4 * width + local_heads]
    )
    beta_gate = jax.nn.sigmoid(summed[:, 4 * width + local_heads :])
    new_state, head_out = delta_update(query, key_vec, value_vec, log_decay, beta_gate, state)
    mixed = head_mix(head_out, head_gain, z_gate).reshape(seq_count, width)
    attn_part = jnp.dot(
        lax.all_gather(mixed, "kv", axis=0, tiled=True),
        w_attn_out,
        preferred_element_type=jnp.float32,
    )
    attn_sum = lax.psum_scatter(
        attn_part.astype(jnp.bfloat16), "tp", scatter_dimension=1, tiled=True
    ).astype(jnp.float32)
    residual_stream = (stream.astype(jnp.float32) + attn_sum).astype(jnp.bfloat16)
    mlp_block = lax.all_gather(residual_stream, "tp", axis=1, tiled=True).astype(jnp.float32)
    mlp_local_squares = jnp.sum(mlp_block * mlp_block, axis=1)
    mlp_total_squares = lax.psum(mlp_local_squares, "kv")
    normed_mlp = (mlp_block * mlp_gain.astype(jnp.float32)[None, :]).astype(jnp.bfloat16)
    gate_part = jnp.dot(normed_mlp, w_gate, preferred_element_type=jnp.float32)
    up_part = jnp.dot(normed_mlp, w_up, preferred_element_type=jnp.float32)
    operands = (gate_part, up_part)
    totals = (
        lax.psum(operands[0].astype(jnp.bfloat16), "kv").astype(jnp.float32),
        lax.psum(operands[1].astype(jnp.bfloat16), "kv").astype(jnp.float32),
    )
    gate_sum, up_sum = (totals[0], totals[1])
    mlp_scale = lax.rsqrt(mlp_total_squares / D + EPSILON)
    hidden = (jax.nn.silu(gate_sum * mlp_scale[:, None]) * (up_sum * mlp_scale[:, None])).astype(
        jnp.bfloat16
    )
    down_part = jnp.dot(hidden, w_down, preferred_element_type=jnp.float32)
    mlp_sum = lax.psum_scatter(
        down_part.astype(jnp.bfloat16), "tp", scatter_dimension=1, tiled=True
    ).astype(jnp.float32)
    next_stream = (residual_stream.astype(jnp.float32) + mlp_sum).astype(jnp.bfloat16)
    return (next_stream, new_state)


LANES = 128
VMEM_BYTES = 67043328
LIMIT = 40 * 1024 * 1024
MESH = pl.DeviceIdType.MESH


def send_slots(count, axis, me, source, slots, send_sem, recv_sem):
    copies = []
    for step in range(1, count):
        peer = lax.rem(me + step, count)
        copy = pltpu.make_async_remote_copy(
            src_ref=source(peer),
            dst_ref=slots.at[me],
            send_sem=send_sem.at[step],
            recv_sem=recv_sem.at[step],
            device_id={axis: peer},
            device_id_type=MESH,
        )
        copy.start()
        copies.append(copy)
    return copies


def wait_slot(count, axis, me, step, slots, send_sem, recv_sem):
    origin = lax.rem(me + count - step, count)
    pltpu.make_async_remote_copy(
        src_ref=slots.at[origin],
        dst_ref=slots.at[origin],
        send_sem=send_sem.at[step],
        recv_sem=recv_sem.at[step],
        device_id={axis: origin},
        device_id_type=MESH,
    ).wait_recv()
    return origin


def layer_kernel(
    kv_count,
    tp_count,
    stream,
    attn_gain,
    mlp_gain,
    w_query,
    w_key,
    w_value,
    w_zgate,
    w_decay,
    w_beta,
    decay_rate,
    head_gain,
    w_attn_out,
    w_gate,
    w_up,
    w_down,
    state,
    out_stream,
    out_state,
    v_query,
    v_key,
    v_value,
    v_zgate,
    v_decay,
    v_beta,
    v_attn_out,
    v_gate,
    v_up,
    v_down,
    v_state,
    x_all,
    normed,
    proj_f,
    proj_b,
    proj_r,
    proj_t,
    rows,
    mix_all,
    mixed_f,
    part_f,
    part_b,
    part_r,
    res_all,
    gu_f,
    gu_b,
    gu_r,
    gu_t,
    hid_all,
    hidden_f,
    down_f,
    down_b,
    down_r,
    next_stream,
    load_sem,
    send_sem,
    recv_sem,
):
    f32, bf16 = jnp.float32, jnp.bfloat16
    kv, tp = lax.axis_index("kv"), lax.axis_index("tp")
    batch, width = stream.shape
    depth, cols = w_query.shape
    seqs, heads = state.shape[0], state.shape[1]
    heads_total = w_decay.shape[0]
    half = w_gate.shape[1] // 2
    features = kv_count * depth

    def load(index, source, target):
        copy = pltpu.make_async_copy(source, target, load_sem.at[index])
        copy.start()
        return copy

    load_x = load(0, stream, x_all.at[tp])
    loads = [
        load(index + 1, source, target)
        for index, (source, target) in enumerate(
            (
                (w_decay, v_decay),
                (w_beta, v_beta),
                (w_query, v_query),
                (w_key, v_key),
                (w_value, v_value),
                (w_zgate, v_zgate),
                (state, v_state),
                (w_attn_out, v_attn_out),
                (w_gate, v_gate),
                (w_up, v_up),
                (w_down, v_down),
            )
        )
    ]
    (l_decay, l_beta, l_query, l_key, l_value, l_zgate) = loads[:6]
    (l_state, l_attn_out, l_gate, l_up, l_down) = loads[6:]

    barrier = pltpu.get_barrier_semaphore()
    for step in range(1, tp_count):
        pl.semaphore_signal(
            barrier, inc=1, device_id={"tp": lax.rem(tp + step, tp_count)}, device_id_type=MESH
        )
    for step in range(1, kv_count):
        pl.semaphore_signal(
            barrier, inc=1, device_id={"kv": lax.rem(kv + step, kv_count)}, device_id_type=MESH
        )
    load_x.wait()
    pl.semaphore_wait(barrier, tp_count - 1 + kv_count - 1)

    def tp_exchange(index, source, slots):
        sends = send_slots(
            tp_count, "tp", tp, source, slots, send_sem.at[index], recv_sem.at[index]
        )

        def arrived(step):
            return wait_slot(
                tp_count, "tp", tp, step, slots, send_sem.at[index], recv_sem.at[index]
            )

        return sends, arrived

    def kv_exchange(index, source, slots):
        sends = send_slots(
            kv_count, "kv", kv, source, slots, send_sem.at[index], recv_sem.at[index]
        )

        def arrived(step):
            return wait_slot(
                kv_count, "kv", kv, step, slots, send_sem.at[index], recv_sem.at[index]
            )

        return sends, arrived

    pending = []

    def norm_inputs(blocks, gain):
        squares = jnp.zeros((batch, 1), f32)
        for t in range(tp_count):
            block = blocks[t].astype(f32)
            squares = squares + jnp.sum(block * block, axis=1, keepdims=True)
            for c in range(0, width, LANES):
                at = t * width + c
                scale = gain[...].astype(f32)[at // LANES : at // LANES + 1]
                normed[:, at : at + LANES] = (block[:, c : c + LANES] * scale).astype(bf16)
        squares = jnp.broadcast_to(squares, (batch, LANES))
        high = squares.astype(bf16).astype(f32)
        return high, squares - high

    sends, arrived = tp_exchange(0, lambda peer: x_all.at[tp], x_all)
    pending += sends
    for step in range(1, tp_count):
        arrived(step)
    high, low = norm_inputs(x_all, attn_gain)

    inputs = normed[...]
    l_decay.wait()
    l_beta.wait()
    by_rows = (((1,), (1,)), ((), ()))
    decay_part = lax.dot_general(inputs, v_decay[...], by_rows, preferred_element_type=f32)
    beta_part = lax.dot_general(inputs, v_beta[...], by_rows, preferred_element_type=f32)
    for j in range(kv_count):
        own = slice(j * seqs, (j + 1) * seqs)
        proj_f[j, :, cols:] = jnp.zeros((4 * seqs, LANES), f32)
        proj_f[j, 0:seqs, cols : cols + heads_total] = decay_part[own]
        proj_f[j, seqs : 2 * seqs, cols : cols + heads_total] = beta_part[own]
        proj_f[j, 2 * seqs : 3 * seqs, cols:] = high[own]
        proj_f[j, 3 * seqs : 4 * seqs, cols:] = low[own]
    for kind, (wait, weight) in enumerate(
        ((l_query, v_query), (l_key, v_key), (l_value, v_value), (l_zgate, v_zgate))
    ):
        wait.wait()
        part = jnp.dot(inputs, weight[...], preferred_element_type=f32)
        for j in range(kv_count):
            proj_f[j, kind * seqs : (kind + 1) * seqs, 0:cols] = part[j * seqs : (j + 1) * seqs]
    for j in range(kv_count):
        proj_b[j] = proj_f[j].astype(bf16)
    sends, arrived = kv_exchange(1, lambda peer: proj_b.at[peer], proj_r)
    pending += sends
    total = proj_f[kv]
    for step in range(1, kv_count):
        total = total + proj_r[arrived(step)].astype(f32)
    proj_t[...] = total

    squares = proj_t[2 * seqs : 3 * seqs, cols:] + proj_t[3 * seqs : 4 * seqs, cols:]
    row_scale = lax.rsqrt(squares / features + EPSILON)
    decay_rows = proj_t[0:seqs, cols:] * row_scale
    beta_rows = proj_t[seqs : 2 * seqs, cols:] * row_scale
    for h in range(heads):
        at = slice(h * seqs, (h + 1) * seqs)
        for kind in range(4):
            rows[kind, at, :] = (
                proj_t[kind * seqs : (kind + 1) * seqs, h * LANES : (h + 1) * LANES] * row_scale
            )
        rows[4, at, :] = decay_rows
        rows[5, at, :] = beta_rows
    count = heads * seqs
    row = lax.broadcasted_iota(jnp.int32, (count, LANES), 0)
    lane = lax.broadcasted_iota(jnp.int32, (count, LANES), 1) - tp * heads
    own_lane = (row >= lane * seqs) & (row < (lane + 1) * seqs)
    decay_pre = jnp.sum(jnp.where(own_lane, rows[4], 0.0), axis=1, keepdims=True)
    beta_pre = jnp.sum(jnp.where(own_lane, rows[5], 0.0), axis=1, keepdims=True)
    row = lax.broadcasted_iota(jnp.int32, (count, heads), 0)
    lane = lax.broadcasted_iota(jnp.int32, (count, heads), 1)
    own_lane = (row >= lane * seqs) & (row < (lane + 1) * seqs)
    rate = jnp.sum(
        jnp.where(own_lane, jnp.broadcast_to(decay_rate[...], (count, heads)), 0.0),
        axis=1,
        keepdims=True,
    )
    softplus = jnp.maximum(decay_pre, 0.0) + jnp.log1p(jnp.exp(-jnp.abs(decay_pre)))
    rows[4] = jnp.broadcast_to(jnp.exp(-rate * softplus), (count, LANES))
    rows[5] = jnp.broadcast_to(jax.nn.sigmoid(beta_pre), (count, LANES))
    query_t = jnp.transpose(l2_unit(rows[0]) * HEAD_DIM ** (-0.5))
    key_t = jnp.transpose(l2_unit(rows[1]))

    l_state.wait()
    for h in range(heads):
        for s in range(seqs):
            i = h * seqs + s
            key_col = key_t[:, i : i + 1]
            decayed = v_state[s, h] * rows[4, i : i + 1, :]
            recalled = jnp.sum(decayed * key_col, axis=0, keepdims=True)
            update = rows[5, i : i + 1, :] * (rows[2, i : i + 1, :] - recalled)
            updated = decayed + key_col * update
            v_state[s, h] = updated
            rows[0, i : i + 1, :] = jnp.sum(
                updated * query_t[:, i : i + 1], axis=0, keepdims=True
            )
    head_out = rows[0]
    scaled = head_out * lax.rsqrt(
        jnp.mean(head_out * head_out, axis=-1, keepdims=True) + EPSILON
    )
    mix_all[kv] = (scaled * head_gain[...] * jax.nn.silu(rows[3])).astype(bf16)
    sends, arrived = kv_exchange(2, lambda peer: mix_all.at[kv], mix_all)
    pending += sends
    store_state = pltpu.make_async_copy(v_state, out_state, load_sem.at[len(loads) + 1])
    store_state.start()
    for step in range(1, kv_count):
        arrived(step)
    for j in range(kv_count):
        mixed = mix_all[j].astype(f32)
        for h in range(heads):
            mixed_f[j * seqs : (j + 1) * seqs, h * LANES : (h + 1) * LANES] = mixed[
                h * seqs : (h + 1) * seqs
            ]

    def sum_over_tp(index, part, held, sent, slots):
        for t in range(tp_count):
            block = part[:, t * width : (t + 1) * width]
            held[t] = block
            sent[t] = block.astype(bf16)
        sends, arrived = tp_exchange(index, lambda peer: sent.at[peer], slots)
        total = held[tp]
        for step in range(1, tp_count):
            total = total + slots[arrived(step)].astype(f32)
        return sends, total

    l_attn_out.wait()
    part = jnp.dot(mixed_f[...].astype(bf16), v_attn_out[...], preferred_element_type=f32)
    sends, attn_sum = sum_over_tp(3, part, part_f, part_b, part_r)
    pending += sends
    res_all[tp] = (x_all[tp].astype(f32) + attn_sum).astype(bf16)
    sends, arrived = tp_exchange(4, lambda peer: res_all.at[tp], res_all)
    pending += sends
    for step in range(1, tp_count):
        arrived(step)
    high, low = norm_inputs(res_all, mlp_gain)

    inputs = normed[...]
    for j in range(kv_count):
        own = slice(j * seqs, (j + 1) * seqs)
        gu_f[j, :, half:] = jnp.zeros((4 * seqs, LANES), f32)
        gu_f[j, 0:seqs, half:] = high[own]
        gu_f[j, seqs : 2 * seqs, half:] = low[own]
    for kind, (wait, weight) in enumerate(((l_gate, v_gate), (l_up, v_up))):
        wait.wait()
        for side in range(2):
            part = jnp.dot(
                inputs,
                weight[:, side * half : (side + 1) * half],
                preferred_element_type=f32,
            )
            at = (2 * kind + side) * seqs
            for j in range(kv_count):
                gu_f[j, at : at + seqs, 0:half] = part[j * seqs : (j + 1) * seqs]
    for j in range(kv_count):
        gu_b[j] = gu_f[j].astype(bf16)
    sends, arrived = kv_exchange(5, lambda peer: gu_b.at[peer], gu_r)
    pending += sends
    total = gu_f[kv]
    for step in range(1, kv_count):
        total = total + gu_r[arrived(step)].astype(f32)
    gu_t[...] = total
    squares = gu_t[0:seqs, half:] + gu_t[seqs : 2 * seqs, half:]
    mlp_scale = lax.rsqrt(squares / features + EPSILON)[:, 0:1]
    mlp_scale = jnp.concatenate([mlp_scale, mlp_scale], axis=0)
    gate = gu_t[0 : 2 * seqs, 0:half] * mlp_scale
    up = gu_t[2 * seqs : 4 * seqs, 0:half] * mlp_scale
    hid_all[kv] = (jax.nn.silu(gate) * up).astype(bf16)
    sends, arrived = kv_exchange(6, lambda peer: hid_all.at[kv], hid_all)
    pending += sends
    for step in range(1, kv_count):
        arrived(step)
    for j in range(kv_count):
        hidden = hid_all[j].astype(f32)
        for side in range(2):
            hidden_f[j * seqs : (j + 1) * seqs, side * half : (side + 1) * half] = hidden[
                side * seqs : (side + 1) * seqs
            ]
    l_down.wait()
    part = jnp.dot(hidden_f[...].astype(bf16), v_down[...], preferred_element_type=f32)
    sends, mlp_sum = sum_over_tp(7, part, down_f, down_b, down_r)
    pending += sends
    next_stream[...] = (res_all[tp].astype(f32) + mlp_sum).astype(bf16)
    store_stream = pltpu.make_async_copy(next_stream, out_stream, load_sem.at[0])
    store_stream.start()
    store_stream.wait()
    for copy in pending:
        copy.wait_send()
    store_state.wait()


def fused(kv_count, tp_count, *args):
    f32, bf16 = jnp.float32, jnp.bfloat16
    (stream, attn_gain, mlp_gain, w_query, w_key, w_value, w_zgate, w_decay, w_beta) = args[:9]
    (decay_rate, head_gain, w_attn_out, w_gate, w_up, w_down, state) = args[9:]
    batch, width = stream.shape
    depth, cols = w_query.shape
    seqs, heads = state.shape[0], state.shape[1]
    half = w_gate.shape[1] // 2
    count = seqs * heads
    steps = max(kv_count, tp_count)
    any_spec = pl.BlockSpec(memory_space=pltpu.HBM)
    vmem_spec = pl.BlockSpec(memory_space=pltpu.VMEM)
    small = jax.ShapeDtypeStruct(w_decay.shape[::-1], w_decay.dtype)
    weights = (w_query, w_key, w_value, w_zgate, small, small, w_attn_out, w_gate, w_up, w_down)
    scratch = [pltpu.VMEM(weight.shape, weight.dtype) for weight in weights + (state,)]
    scratch += [
        pltpu.VMEM((tp_count, batch, width), bf16),
        pltpu.VMEM((batch, depth), bf16),
        pltpu.VMEM((kv_count, 4 * seqs, cols + LANES), f32),
        pltpu.VMEM((kv_count, 4 * seqs, cols + LANES), bf16),
        pltpu.VMEM((kv_count, 4 * seqs, cols + LANES), bf16),
        pltpu.VMEM((4 * seqs, cols + LANES), f32),
        pltpu.VMEM((6, count, LANES), f32),
        pltpu.VMEM((kv_count, count, LANES), bf16),
        pltpu.VMEM((batch, cols), f32),
        pltpu.VMEM((tp_count, batch, width), f32),
        pltpu.VMEM((tp_count, batch, width), bf16),
        pltpu.VMEM((tp_count, batch, width), bf16),
        pltpu.VMEM((tp_count, batch, width), bf16),
        pltpu.VMEM((kv_count, 4 * seqs, half + LANES), f32),
        pltpu.VMEM((kv_count, 4 * seqs, half + LANES), bf16),
        pltpu.VMEM((kv_count, 4 * seqs, half + LANES), bf16),
        pltpu.VMEM((4 * seqs, half + LANES), f32),
        pltpu.VMEM((kv_count, 2 * seqs, half), bf16),
        pltpu.VMEM((batch, 2 * half), f32),
        pltpu.VMEM((tp_count, batch, width), f32),
        pltpu.VMEM((tp_count, batch, width), bf16),
        pltpu.VMEM((tp_count, batch, width), bf16),
        pltpu.VMEM((batch, width), bf16),
        pltpu.SemaphoreType.DMA((13,)),
        pltpu.SemaphoreType.DMA((8, steps)),
        pltpu.SemaphoreType.DMA((8, steps)),
    ]
    outs = pl.pallas_call(
        functools.partial(layer_kernel, kv_count, tp_count),
        out_shape=(pltpu.VMEM(stream.shape, bf16), pltpu.VMEM(state.shape, f32)),
        in_specs=[any_spec]
        + [vmem_spec] * 2
        + [any_spec] * 6
        + [vmem_spec] * 2
        + [any_spec] * 5,
        out_specs=(pl.BlockSpec(memory_space=pl.ANY),) * 2,
        scratch_shapes=scratch,
        compiler_params=pltpu.CompilerParams(
            collective_id=0, has_side_effects=True, vmem_limit_bytes=LIMIT
        ),
    )(
        *map(in_hbm, (
        stream,
        attn_gain.reshape(-1, LANES),
        mlp_gain.reshape(-1, LANES),
        w_query,
        w_key,
        w_value,
        w_zgate,
        w_decay.T,
        w_beta.T,
        decay_rate.reshape(1, -1),
        head_gain.reshape(1, -1),
        w_attn_out,
        w_gate,
        w_up,
        w_down,
        state,
        ))
    )
    return pl.pallas_call(
        finish_kernel,
        out_shape=tuple(jax.ShapeDtypeStruct(out.shape, out.dtype) for out in outs),
        in_specs=[pl.BlockSpec(memory_space=pl.ANY)] * 2,
        out_specs=(any_spec,) * 2,
        scratch_shapes=[pltpu.SemaphoreType.DMA((2,))],
        compiler_params=pltpu.CompilerParams(vmem_limit_bytes=1024 * 1024),
    )(*outs)


def in_hbm(array):
    return pltpu.with_memory_space_constraint(array, pltpu.HBM)


def finish_kernel(stream, state, out_stream, out_state, sem):
    copies = [
        pltpu.make_async_copy(state, out_state, sem.at[0]),
        pltpu.make_async_copy(stream, out_stream, sem.at[1]),
    ]
    for copy in copies:
        copy.start()
    for copy in copies:
        copy.wait()


def layer(mesh, *args):
    kv_count, tp_count = mesh.shape["kv"], mesh.shape["tp"]
    stream, w_query, w_gate, state = args[0], args[3], args[12], args[15]
    seqs, heads = state.shape[0], state.shape[1]
    held = sum(math.prod(a.shape) * a.dtype.itemsize for a in args)
    tiled = (
        stream.shape[1] % LANES == 0
        and w_query.shape[0] == tp_count * stream.shape[1]
        and stream.shape[0] == kv_count * seqs
        and stream.shape[0] % 16 == 0
        and (2 * seqs) % 8 == 0
        and (seqs * heads) % 16 == 0
        and w_gate.shape[1] % (2 * LANES) == 0
        and args[7].shape[1] <= LANES
        and state.shape[2] == LANES
        and state.shape[3] == LANES
        and kv_count > 1
        and tp_count > 1
        and held < VMEM_BYTES * 3 // 4
    )
    if tiled:
        return fused(kv_count, tp_count, *args)
    return local(*args)


def solution(mesh):
    return jax.shard_map(
        functools.partial(layer, mesh),
        mesh=mesh,
        in_specs=(
            P("grp", ("kv", "tp")),
            P("kv"),
            P("kv"),
            P("kv", "tp"),
            P("kv", "tp"),
            P("kv", "tp"),
            P("kv", "tp"),
            P("kv", None),
            P("kv", None),
            P("tp"),
            P(),
            P("tp", "kv"),
            P("kv", "tp"),
            P("kv", "tp"),
            P("tp", "kv"),
            P(("grp", "kv"), "tp", None, None),
        ),
        out_specs=(P("grp", ("kv", "tp")), P(("grp", "kv"), "tp", None, None)),
        check_vma=False,
    )
```

```python
import functools
import math

import jax
import jax.numpy as jnp
from jax import lax
from jax.experimental import pallas as pl
from jax.experimental.pallas import tpu as pltpu
from jax.sharding import PartitionSpec as P

D = 4096
HEAD_DIM = 128


EPSILON = 1e-06


def l2_unit(values):
    return values * lax.rsqrt(jnp.sum(values * values, axis=-1, keepdims=True) + EPSILON)


def delta_update(query, key_vec, value_vec, log_decay, beta_gate, state):
    decayed = jnp.exp(log_decay)[..., None, None] * state
    recalled = jnp.einsum("shkv,shk->shv", decayed, key_vec, precision=lax.Precision.HIGHEST)
    update = beta_gate[..., None] * (value_vec - recalled)
    new_state = decayed + key_vec[..., :, None] * update[..., None, :]
    head_out = jnp.einsum("shkv,shk->shv", new_state, query, precision=lax.Precision.HIGHEST)
    return (new_state, head_out)


def head_mix(head_out, head_gain, z_gate):
    scaled = head_out * lax.rsqrt(jnp.mean(head_out * head_out, axis=-1, keepdims=True) + EPSILON)
    return (scaled * head_gain * jax.nn.silu(z_gate)).astype(jnp.bfloat16)


def local(
    stream,
    attn_gain,
    mlp_gain,
    w_query,
    w_key,
    w_value,
    w_zgate,
    w_decay,
    w_beta,
    decay_rate,
    head_gain,
    w_attn_out,
    w_gate,
    w_up,
    w_down,
    state,
):
    seq_count = state.shape[0]
    local_heads = state.shape[1]
    width = w_query.shape[1]
    heads_total = w_decay.shape[1]
    kv_offset = lax.axis_index("kv") * seq_count
    head_offset = lax.axis_index("tp") * local_heads
    block_rows = lax.all_gather(stream, "tp", axis=1, tiled=True).astype(jnp.float32)
    local_squares = jnp.sum(block_rows * block_rows, axis=1)
    normed = (block_rows * attn_gain.astype(jnp.float32)[None, :]).astype(jnp.bfloat16)
    small_weights = jnp.concatenate([w_decay, w_beta], axis=1)
    pieces = [
        jnp.dot(normed, weight, preferred_element_type=jnp.float32)
        for weight in (w_query, w_key, w_value, w_zgate)
    ]
    small = jnp.dot(normed, small_weights, preferred_element_type=jnp.float32)
    own_decay = lax.dynamic_slice_in_dim(small, head_offset, local_heads, 1)
    own_beta = lax.dynamic_slice_in_dim(small, heads_total + head_offset, local_heads, 1)
    summed = lax.psum_scatter(
        jnp.concatenate(pieces + [own_decay, own_beta], axis=1).astype(jnp.bfloat16),
        "kv",
        scatter_dimension=0,
        tiled=True,
    ).astype(jnp.float32)
    total_squares = lax.psum(local_squares, "kv")
    row_scale = lax.rsqrt(total_squares / D + EPSILON)
    own_scale = lax.dynamic_slice_in_dim(row_scale, kv_offset, seq_count, 0)
    summed = summed * own_scale[:, None]

    def head_block(index):
        return summed[:, index * width : (index + 1) * width].reshape(
            seq_count, local_heads, HEAD_DIM
        )

    query = l2_unit(head_block(0)) * HEAD_DIM ** (-0.5)
    key_vec = l2_unit(head_block(1))
    value_vec = head_block(2)
    z_gate = head_block(3)
    log_decay = -decay_rate[None, :] * jax.nn.softplus(
        summed[:, 4 * width : 4 * width + local_heads]
    )
    beta_gate = jax.nn.sigmoid(summed[:, 4 * width + local_heads :])
    new_state, head_out = delta_update(query, key_vec, value_vec, log_decay, beta_gate, state)
    mixed = head_mix(head_out, head_gain, z_gate).reshape(seq_count, width)
    attn_part = jnp.dot(
        lax.all_gather(mixed, "kv", axis=0, tiled=True),
        w_attn_out,
        preferred_element_type=jnp.float32,
    )
    attn_sum = lax.psum_scatter(
        attn_part.astype(jnp.bfloat16), "tp", scatter_dimension=1, tiled=True
    ).astype(jnp.float32)
    residual_stream = (stream.astype(jnp.float32) + attn_sum).astype(jnp.bfloat16)
    mlp_block = lax.all_gather(residual_stream, "tp", axis=1, tiled=True).astype(jnp.float32)
    mlp_local_squares = jnp.sum(mlp_block * mlp_block, axis=1)
    mlp_total_squares = lax.psum(mlp_local_squares, "kv")
    normed_mlp = (mlp_block * mlp_gain.astype(jnp.float32)[None, :]).astype(jnp.bfloat16)
    gate_part = jnp.dot(normed_mlp, w_gate, preferred_element_type=jnp.float32)
    up_part = jnp.dot(normed_mlp, w_up, preferred_element_type=jnp.float32)
    operands = (gate_part, up_part)
    totals = (
        lax.psum(operands[0].astype(jnp.bfloat16), "kv").astype(jnp.float32),
        lax.psum(operands[1].astype(jnp.bfloat16), "kv").astype(jnp.float32),
    )
    gate_sum, up_sum = (totals[0], totals[1])
    mlp_scale = lax.rsqrt(mlp_total_squares / D + EPSILON)
    hidden = (jax.nn.silu(gate_sum * mlp_scale[:, None]) * (up_sum * mlp_scale[:, None])).astype(
        jnp.bfloat16
    )
    down_part = jnp.dot(hidden, w_down, preferred_element_type=jnp.float32)
    mlp_sum = lax.psum_scatter(
        down_part.astype(jnp.bfloat16), "tp", scatter_dimension=1, tiled=True
    ).astype(jnp.float32)
    next_stream = (residual_stream.astype(jnp.float32) + mlp_sum).astype(jnp.bfloat16)
    return (next_stream, new_state)


LANES = 128
VMEM_BYTES = 67043328
LIMIT = 40 * 1024 * 1024
MESH = pl.DeviceIdType.MESH


def partner(count, me, step):
    upper = lax.div(2 * me, count)
    falling = count - 1 - step - lax.div(me + step + 1, count)
    rising = step + lax.div(step + count - me, count)
    return upper * rising + (1 - upper) * falling


def send_slots(count, axis, me, source, target, send_sem, recv_sem):
    copies = []
    for step in range(count - 1):
        peer = partner(count, me, step)
        copy = pltpu.make_async_remote_copy(
            src_ref=source(peer),
            dst_ref=target(me),
            send_sem=send_sem.at[step],
            recv_sem=recv_sem.at[me],
            device_id={axis: peer},
            device_id_type=MESH,
        )
        copy.start()
        copies.append(copy)
    return copies


def wait_slot(count, axis, me, step, target, send_sem, recv_sem):
    origin = partner(count, me, count - 2 - step)
    pltpu.make_async_remote_copy(
        src_ref=target(origin),
        dst_ref=target(origin),
        send_sem=send_sem.at[step],
        recv_sem=recv_sem.at[origin],
        device_id={axis: origin},
        device_id_type=MESH,
    ).wait_recv()
    return origin


def layer_kernel(
    kv_count,
    tp_count,
    stream,
    attn_gain,
    mlp_gain,
    w_query,
    w_key,
    w_value,
    w_zgate,
    w_decay,
    w_beta,
    decay_rate,
    head_gain,
    w_attn_out,
    w_gate,
    w_up,
    w_down,
    state,
    out_stream,
    out_state,
    v_query,
    v_key,
    v_value,
    v_zgate,
    v_decay,
    v_beta,
    v_attn_out,
    v_gate,
    v_up,
    v_down,
    v_state,
    x_all,
    normed,
    proj_f,
    proj_b,
    proj_r,
    proj_t,
    rows,
    mix_all,
    mixed_f,
    part_b,
    res_all,
    gu_f,
    gu_b,
    gu_r,
    gu_t,
    hid_all,
    hidden_f,
    down_f,
    down_b,
    down_r,
    next_stream,
    g_attn,
    g_mlp,
    v_rate,
    g_head,
    load_sem,
    send_sem,
    recv_sem,
):
    f32, bf16 = jnp.float32, jnp.bfloat16
    kv, tp = lax.axis_index("kv"), lax.axis_index("tp")
    batch, width = stream.shape
    depth, cols = w_query.shape
    seqs, heads = state.shape[0], state.shape[1]
    heads_total = w_decay.shape[0]
    half = w_gate.shape[1] // 2
    features = kv_count * depth

    barrier = pltpu.get_barrier_semaphore()
    for step in range(1, tp_count):
        pl.semaphore_signal(
            barrier, inc=1, device_id={"tp": lax.rem(tp + step, tp_count)}, device_id_type=MESH
        )
    for step in range(1, kv_count):
        pl.semaphore_signal(
            barrier, inc=1, device_id={"kv": lax.rem(kv + step, kv_count)}, device_id_type=MESH
        )

    def load(index, source, target):
        copy = pltpu.make_async_copy(source, target, load_sem.at[index])
        copy.start()
        return copy

    load_x = load(0, stream, x_all.at[tp])
    loads = [
        load(index + 1, source, target)
        for index, (source, target) in enumerate(
            (
                (attn_gain, g_attn),
                (mlp_gain, g_mlp),
                (decay_rate, v_rate),
                (head_gain, g_head),
                (w_decay, v_decay),
                (w_beta, v_beta),
                (w_query, v_query),
                (w_key, v_key),
                (w_value, v_value),
                (w_zgate, v_zgate),
                (state, v_state),
                (w_attn_out, v_attn_out),
                (w_gate, v_gate),
                (w_up, v_up),
                (w_down, v_down),
            )
        )
    ]
    (l_decay, l_beta, l_query, l_key, l_value, l_zgate) = loads[4:10]
    (l_state, l_attn_out, l_gate, l_up, l_down) = loads[10:]

    load_x.wait()
    pl.semaphore_wait(barrier, tp_count - 1 + kv_count - 1)

    pending = []

    def exchange(count, axis, me, index, source, target):
        sems = send_sem.at[index], recv_sem.at[index]
        pending.extend(send_slots(count, axis, me, source, target, *sems))

        def arrived(step):
            return wait_slot(count, axis, me, step, target, *sems)

        return arrived

    tp_exchange = functools.partial(exchange, tp_count, "tp", tp)
    kv_exchange = functools.partial(exchange, kv_count, "kv", kv)

    def norm_inputs(blocks, gain):
        squares = jnp.zeros((batch, 1), f32)
        for t in range(tp_count):
            block = blocks[t].astype(f32)
            squares = squares + jnp.sum(block * block, axis=1, keepdims=True)
            for c in range(0, width, LANES):
                at = t * width + c
                scale = gain[...].astype(f32)[at // LANES : at // LANES + 1]
                normed[:, at : at + LANES] = (block[:, c : c + LANES] * scale).astype(bf16)
        squares = jnp.broadcast_to(squares, (batch, LANES))
        high = squares.astype(bf16).astype(f32)
        return high, squares - high

    arrived = tp_exchange(0, lambda peer: x_all.at[tp], lambda slot: x_all.at[slot])
    for step in range(tp_count - 1):
        arrived(step)
    for small in loads[:4]:
        small.wait()
    high, low = norm_inputs(x_all, g_attn)

    inputs = normed[...]
    l_decay.wait()
    l_beta.wait()
    by_rows = (((1,), (1,)), ((), ()))
    decay_part = lax.dot_general(inputs, v_decay[...], by_rows, preferred_element_type=f32)
    beta_part = lax.dot_general(inputs, v_beta[...], by_rows, preferred_element_type=f32)
    for j in range(kv_count):
        own = slice(j * seqs, (j + 1) * seqs)
        proj_f[j, :, cols:] = jnp.zeros((4 * seqs, LANES), f32)
        proj_f[j, 0:seqs, cols : cols + heads_total] = decay_part[own]
        proj_f[j, seqs : 2 * seqs, cols : cols + heads_total] = beta_part[own]
        proj_f[j, 2 * seqs : 3 * seqs, cols:] = high[own]
        proj_f[j, 3 * seqs : 4 * seqs, cols:] = low[own]
    projections = ((l_query, v_query), (l_key, v_key), (l_value, v_value), (l_zgate, v_zgate))
    arrivals = []
    for side in range(2):
        at = pl.ds(2 * side * seqs, 2 * seqs)
        for kind in (2 * side, 2 * side + 1):
            wait, weight = projections[kind]
            wait.wait()
            part = jnp.dot(inputs, weight[...], preferred_element_type=f32)
            for j in range(kv_count):
                proj_f[j, kind * seqs : (kind + 1) * seqs, 0:cols] = part[
                    j * seqs : (j + 1) * seqs
                ]
        for j in range(kv_count):
            proj_b[j, at] = proj_f[j, at].astype(bf16)
        arrivals.append(
            kv_exchange(
                1 + side,
                lambda peer, at=at: proj_b.at[peer, at],
                lambda slot, at=at: proj_r.at[slot, at],
            )
        )
    total = proj_f[kv]
    for step in range(kv_count - 1):
        for arrived in arrivals:
            origin = arrived(step)
        total = total + proj_r[origin].astype(f32)
    proj_t[...] = total

    squares = proj_t[2 * seqs : 3 * seqs, cols:] + proj_t[3 * seqs : 4 * seqs, cols:]
    row_scale = lax.rsqrt(squares / features + EPSILON)
    decay_rows = proj_t[0:seqs, cols:] * row_scale
    beta_rows = proj_t[seqs : 2 * seqs, cols:] * row_scale
    for h in range(heads):
        at = slice(h * seqs, (h + 1) * seqs)
        for kind in range(4):
            rows[kind, at, :] = (
                proj_t[kind * seqs : (kind + 1) * seqs, h * LANES : (h + 1) * LANES] * row_scale
            )
        rows[4, at, :] = decay_rows
        rows[5, at, :] = beta_rows
    count = heads * seqs
    row = lax.broadcasted_iota(jnp.int32, (count, LANES), 0)
    lane = lax.broadcasted_iota(jnp.int32, (count, LANES), 1) - tp * heads
    own_lane = (row >= lane * seqs) & (row < (lane + 1) * seqs)
    decay_pre = jnp.sum(jnp.where(own_lane, rows[4], 0.0), axis=1, keepdims=True)
    beta_pre = jnp.sum(jnp.where(own_lane, rows[5], 0.0), axis=1, keepdims=True)
    row = lax.broadcasted_iota(jnp.int32, (count, heads), 0)
    lane = lax.broadcasted_iota(jnp.int32, (count, heads), 1)
    own_lane = (row >= lane * seqs) & (row < (lane + 1) * seqs)
    rate = jnp.sum(
        jnp.where(own_lane, jnp.broadcast_to(v_rate[...], (count, heads)), 0.0),
        axis=1,
        keepdims=True,
    )
    softplus = jnp.maximum(decay_pre, 0.0) + jnp.log1p(jnp.exp(-jnp.abs(decay_pre)))
    rows[4] = jnp.broadcast_to(jnp.exp(-rate * softplus), (count, LANES))
    rows[5] = jnp.broadcast_to(jax.nn.sigmoid(beta_pre), (count, LANES))
    query_t = jnp.transpose(l2_unit(rows[0]) * HEAD_DIM ** (-0.5))
    key_t = jnp.transpose(l2_unit(rows[1]))

    l_state.wait()
    for h in range(heads):
        for s in range(seqs):
            i = h * seqs + s
            key_col = key_t[:, i : i + 1]
            decayed = v_state[s, h] * rows[4, i : i + 1, :]
            recalled = jnp.sum(decayed * key_col, axis=0, keepdims=True)
            update = rows[5, i : i + 1, :] * (rows[2, i : i + 1, :] - recalled)
            updated = decayed + key_col * update
            v_state[s, h] = updated
            rows[0, i : i + 1, :] = jnp.sum(
                updated * query_t[:, i : i + 1], axis=0, keepdims=True
            )
    head_out = rows[0]
    scaled = head_out * lax.rsqrt(
        jnp.mean(head_out * head_out, axis=-1, keepdims=True) + EPSILON
    )
    mix_all[kv] = (scaled * g_head[...] * jax.nn.silu(rows[3])).astype(bf16)
    arrived = kv_exchange(3, lambda peer: mix_all.at[kv], lambda slot: mix_all.at[slot])
    store_state = pltpu.make_async_copy(v_state, out_state, load_sem.at[len(loads) + 1])
    store_state.start()
    for step in range(kv_count - 1):
        arrived(step)
    for j in range(kv_count):
        mixed = mix_all[j].astype(f32)
        for h in range(heads):
            mixed_f[j * seqs : (j + 1) * seqs, h * LANES : (h + 1) * LANES] = mixed[
                h * seqs : (h + 1) * seqs
            ]

    l_attn_out.wait()
    part_b[tp] = jnp.dot(
        mixed_f[...].astype(bf16), v_attn_out[...], preferred_element_type=f32
    ).astype(bf16)
    arrived = tp_exchange(4, lambda peer: part_b.at[tp], lambda slot: part_b.at[slot])
    for step in range(tp_count - 1):
        arrived(step)
    total = part_b[0].astype(f32)
    for t in range(1, tp_count):
        total = total + part_b[t].astype(f32)
    for t in range(tp_count):
        res_all[t] = (
            x_all[t].astype(f32) + total[:, t * width : (t + 1) * width]
        ).astype(bf16)
    high, low = norm_inputs(res_all, g_mlp)

    inputs = normed[...]
    for j in range(kv_count):
        own = slice(j * seqs, (j + 1) * seqs)
        gu_f[j, :, half:] = jnp.zeros((4 * seqs, LANES), f32)
        gu_f[j, 0:seqs, half:] = high[own]
        gu_f[j, seqs : 2 * seqs, half:] = low[own]
    arrivals = []
    for kind, (wait, weight) in enumerate(((l_gate, v_gate), (l_up, v_up))):
        wait.wait()
        for side in range(2):
            part = jnp.dot(
                inputs,
                weight[:, side * half : (side + 1) * half],
                preferred_element_type=f32,
            )
            at = (2 * kind + side) * seqs
            for j in range(kv_count):
                gu_f[j, at : at + seqs, 0:half] = part[j * seqs : (j + 1) * seqs]
        at = pl.ds(2 * kind * seqs, 2 * seqs)
        for j in range(kv_count):
            gu_b[j, at] = gu_f[j, at].astype(bf16)
        arrivals.append(
            kv_exchange(
                5 + kind,
                lambda peer, at=at: gu_b.at[peer, at],
                lambda slot, at=at: gu_r.at[slot, at],
            )
        )
    total = gu_f[kv]
    for step in range(kv_count - 1):
        for arrived in arrivals:
            origin = arrived(step)
        total = total + gu_r[origin].astype(f32)
    gu_t[...] = total
    squares = gu_t[0:seqs, half:] + gu_t[seqs : 2 * seqs, half:]
    mlp_scale = lax.rsqrt(squares / features + EPSILON)[:, 0:1]
    mlp_scale = jnp.concatenate([mlp_scale, mlp_scale], axis=0)
    gate = gu_t[0 : 2 * seqs, 0:half] * mlp_scale
    up = gu_t[2 * seqs : 4 * seqs, 0:half] * mlp_scale
    hid_all[kv] = (jax.nn.silu(gate) * up).astype(bf16)
    arrived = kv_exchange(7, lambda peer: hid_all.at[kv], lambda slot: hid_all.at[slot])
    for step in range(kv_count - 1):
        arrived(step)
    for j in range(kv_count):
        hidden = hid_all[j].astype(f32)
        for side in range(2):
            hidden_f[j * seqs : (j + 1) * seqs, side * half : (side + 1) * half] = hidden[
                side * seqs : (side + 1) * seqs
            ]
    l_down.wait()
    part = jnp.dot(hidden_f[...].astype(bf16), v_down[...], preferred_element_type=f32)
    for t in range(tp_count):
        block = part[:, t * width : (t + 1) * width]
        down_f[t] = block
        down_b[t] = block.astype(bf16)
    arrived = tp_exchange(8, lambda peer: down_b.at[peer], lambda slot: down_r.at[slot])
    mlp_sum = down_f[tp]
    for step in range(tp_count - 1):
        mlp_sum = mlp_sum + down_r[arrived(step)].astype(f32)
    next_stream[...] = (res_all[tp].astype(f32) + mlp_sum).astype(bf16)
    store_stream = pltpu.make_async_copy(next_stream, out_stream, load_sem.at[0])
    store_stream.start()
    store_stream.wait()
    for copy in pending:
        copy.wait_send()
    store_state.wait()


def fused(kv_count, tp_count, *args):
    f32, bf16 = jnp.float32, jnp.bfloat16
    (stream, attn_gain, mlp_gain, w_query, w_key, w_value, w_zgate, w_decay, w_beta) = args[:9]
    (decay_rate, head_gain, w_attn_out, w_gate, w_up, w_down, state) = args[9:]
    batch, width = stream.shape
    depth, cols = w_query.shape
    seqs, heads = state.shape[0], state.shape[1]
    half = w_gate.shape[1] // 2
    count = seqs * heads
    steps = max(kv_count, tp_count)
    any_spec = pl.BlockSpec(memory_space=pltpu.HBM)
    small = jax.ShapeDtypeStruct(w_decay.shape[::-1], w_decay.dtype)
    weights = (w_query, w_key, w_value, w_zgate, small, small, w_attn_out, w_gate, w_up, w_down)
    scratch = [pltpu.VMEM(weight.shape, weight.dtype) for weight in weights + (state,)]
    scratch += [
        pltpu.VMEM((tp_count, batch, width), bf16),
        pltpu.VMEM((batch, depth), bf16),
        pltpu.VMEM((kv_count, 4 * seqs, cols + LANES), f32),
        pltpu.VMEM((kv_count, 4 * seqs, cols + LANES), bf16),
        pltpu.VMEM((kv_count, 4 * seqs, cols + LANES), bf16),
        pltpu.VMEM((4 * seqs, cols + LANES), f32),
        pltpu.VMEM((6, count, LANES), f32),
        pltpu.VMEM((kv_count, count, LANES), bf16),
        pltpu.VMEM((batch, cols), f32),
        pltpu.VMEM((tp_count, batch, tp_count * width), bf16),
        pltpu.VMEM((tp_count, batch, width), bf16),
        pltpu.VMEM((kv_count, 4 * seqs, half + LANES), f32),
        pltpu.VMEM((kv_count, 4 * seqs, half + LANES), bf16),
        pltpu.VMEM((kv_count, 4 * seqs, half + LANES), bf16),
        pltpu.VMEM((4 * seqs, half + LANES), f32),
        pltpu.VMEM((kv_count, 2 * seqs, half), bf16),
        pltpu.VMEM((batch, 2 * half), f32),
        pltpu.VMEM((tp_count, batch, width), f32),
        pltpu.VMEM((tp_count, batch, width), bf16),
        pltpu.VMEM((tp_count, batch, width), bf16),
        pltpu.VMEM((batch, width), bf16),
        pltpu.VMEM((depth // LANES, LANES), bf16),
        pltpu.VMEM((depth // LANES, LANES), bf16),
        pltpu.VMEM((1, heads), f32),
        pltpu.VMEM((1, LANES), f32),
        pltpu.SemaphoreType.DMA((17,)),
        pltpu.SemaphoreType.DMA((9, steps)),
        pltpu.SemaphoreType.DMA((9, steps)),
    ]
    outs = pl.pallas_call(
        functools.partial(layer_kernel, kv_count, tp_count),
        out_shape=(pltpu.VMEM(stream.shape, bf16), pltpu.VMEM(state.shape, f32)),
        in_specs=[any_spec] * len(args),
        out_specs=(pl.BlockSpec(memory_space=pl.ANY),) * 2,
        scratch_shapes=scratch,
        compiler_params=pltpu.CompilerParams(
            collective_id=0, has_side_effects=True, vmem_limit_bytes=LIMIT
        ),
    )(
        *map(in_hbm, (
        stream,
        attn_gain.reshape(-1, LANES),
        mlp_gain.reshape(-1, LANES),
        w_query,
        w_key,
        w_value,
        w_zgate,
        w_decay.T,
        w_beta.T,
        decay_rate.reshape(1, -1),
        head_gain.reshape(1, -1),
        w_attn_out,
        w_gate,
        w_up,
        w_down,
        state,
        ))
    )
    return pl.pallas_call(
        finish_kernel,
        out_shape=tuple(jax.ShapeDtypeStruct(out.shape, out.dtype) for out in outs),
        in_specs=[pl.BlockSpec(memory_space=pl.ANY)] * 2,
        out_specs=(any_spec,) * 2,
        scratch_shapes=[pltpu.SemaphoreType.DMA((2,))],
        compiler_params=pltpu.CompilerParams(vmem_limit_bytes=1024 * 1024),
    )(*outs)


def in_hbm(array):
    return pltpu.with_memory_space_constraint(array, pltpu.HBM)


def finish_kernel(stream, state, out_stream, out_state, sem):
    copies = [
        pltpu.make_async_copy(state, out_state, sem.at[0]),
        pltpu.make_async_copy(stream, out_stream, sem.at[1]),
    ]
    for copy in copies:
        copy.start()
    for copy in copies:
        copy.wait()


def layer(mesh, *args):
    kv_count, tp_count = mesh.shape["kv"], mesh.shape["tp"]
    stream, w_query, w_gate, state = args[0], args[3], args[12], args[15]
    seqs, heads = state.shape[0], state.shape[1]
    held = sum(math.prod(a.shape) * a.dtype.itemsize for a in args)
    tiled = (
        stream.shape[1] % LANES == 0
        and w_query.shape[0] == tp_count * stream.shape[1]
        and args[11].shape[1] == tp_count * stream.shape[1]
        and stream.shape[0] == kv_count * seqs
        and stream.shape[0] % 16 == 0
        and (2 * seqs) % 8 == 0
        and (seqs * heads) % 16 == 0
        and w_gate.shape[1] % (2 * LANES) == 0
        and args[7].shape[1] <= LANES
        and state.shape[2] == LANES
        and state.shape[3] == LANES
        and kv_count > 1
        and tp_count > 1
        and held < VMEM_BYTES * 3 // 4
    )
    if tiled:
        return fused(kv_count, tp_count, *args)
    return local(*args)


def solution(mesh):
    return jax.shard_map(
        functools.partial(layer, mesh),
        mesh=mesh,
        in_specs=(
            P("grp", ("kv", "tp")),
            P("kv"),
            P("kv"),
            P("kv", "tp"),
            P("kv", "tp"),
            P("kv", "tp"),
            P("kv", "tp"),
            P("kv", None),
            P("kv", None),
            P("tp"),
            P(),
            P("tp", "kv"),
            P("kv", "tp"),
            P("kv", "tp"),
            P("tp", "kv"),
            P(("grp", "kv"), "tp", None, None),
        ),
        out_specs=(P("grp", ("kv", "tp")), P(("grp", "kv"), "tp", None, None)),
        check_vma=False,
    )
```
